32 devices in a mesh: grp: 2 (over x), ep: 16 (over z, y, core).
Axes of the slice: x: 2, y: 2, z: 4, core: 2. Of those that a mesh axis runs over, the one named last changes fastest.
Arguments:
- tokens: bfloat16 [2048, 2048], P(('grp', 'ep')), parts along dimension 0, may hold values from -6 to 6
- lengths: int32 [256], P(('grp', 'ep')), parts along dimension 0, may hold values from 1 to 8, 384 in all
- experts: int32 [2048, 2], P(('grp', 'ep')), parts along dimension 0, may hold values from 0 to 3, all different within a row; in each aligned block of 64 rows (0 to 63, 64 to 127, ...) at most 64 rows name the same one
- route_weights: float32 [2048, 2], P(('grp', 'ep')), parts along dimension 0, may hold values from 0.2 to 1
- gate_proj: bfloat16 [16, 2048, 1792], P('ep'), may hold values from -0.125 to 0.125
- up_proj: bfloat16 [16, 2048, 1792], P('ep'), may hold values from -0.125 to 0.125
- down_proj: bfloat16 [16, 1792, 2048], P('ep'), may hold values from -0.0625 to 0.0625
- norm_gain: float32 [2048], replicated, may hold values from 0.1 to 1.9
- norm_bias: float32 [2048], replicated, may hold values from -3 to 3
Outputs:
- mixed: bfloat16 [2048, 2048], P(('grp', 'ep')), parts along dimension 0
The draws below stay inside these ranges and needn't reach their ends.
There are 2 independent parts, one for each index of `grp`. The reference program is written for one: setup_inputs(seed, part) draws one part's arguments, and reference() takes and returns one part's arrays. A program takes and returns all parts, laid end to end along the dimension named above; an argument that names none is the same for every part. Nothing has to cross between parts.
Inputs may be any that keep to these rules, and one draw needn't show every extreme that they name: Each row names 2 different experts; in the rows of one device (aligned blocks of 64 rows) no expert is named by more than 64 rows. Within each copy of the problem the 128 lengths sum to 384; the whole array, over all copies, sums to that times the number of copies.
All inputs are finite; a program needn't handle non-finite values. No bound on the sum of `lengths` on one device may be relied on, other than what follows from the above.
Results may differ from the reference program's by a relative error of at most 0.0021.
Values may be sent and summed in bfloat16 or wider, within the bound.
A program may use at most 128 MiB of HBM per device.

```python
import math
import jax
import jax.numpy as jnp
import numpy as np
from jax import lax

D = 2048
FF = 7168
SPLIT = 4
TOP = 2
SPAN = 8
EXPERTS = 4
FF_DEV = 1792
SLOTS_DEV = 64
SEQS = 128
SLOTS = 1024
CAP = 64
N_EP = 16


def levels(key, dims, cuts, least, largest):
    gain = 1.0
    for dim, parts in cuts:
        heights = jax.random.uniform(jax.random.fold_in(jax.random.fold_in(key, 6), dim), (parts,), jnp.float32, least / len(cuts), largest / len(cuts))
        gain = gain * jnp.repeat(jnp.exp(heights), dims[dim] // parts).reshape((-1,) + (1,) * (len(dims) - 1 - dim))
    return gain


def length_profile(number_of, total, limit, slope):
    portions = [(1 << 20) // math.isqrt(rank ** slope) + 1 for rank in range(2, number_of + 1)]
    surplus, given = total - limit - (number_of - 1), [1] * (number_of - 1)
    while surplus > 0:
        movable = [i for i in range(number_of - 1) if given[i] < limit]
        mass, left = sum([portions[i] for i in movable]), surplus
        for i in movable:
            extra = min(limit - given[i], max(1, left * portions[i] // mass), surplus)
            given[i] = given[i] + extra
            surplus = surplus - extra
    return np.array([limit] + given)


def uneven(key, amount, total, limit, skew):
    if amount == 2:
        one = jax.random.randint(key, (), max(1, total - limit), min(limit, total - 1) + 1)
        return jnp.stack([one, total - one])
    tallies = jnp.asarray(length_profile(amount, total, limit, skew), jnp.int32)
    couples = (amount - 1) // 2
    donor, sink = tallies[1:1 + 2 * couples:2], tallies[2:2 + 2 * couples:2]
    margin = jnp.minimum(donor - 1, limit - sink)
    moved = jax.random.randint(jax.random.fold_in(key, 1), (couples,), 0, 1 << 20) % (margin + 1)
    tallies = tallies.at[1:1 + 2 * couples:2].set(donor - moved).at[2:2 + 2 * couples:2].set(sink + moved)
    return tallies[jax.random.permutation(jax.random.fold_in(key, 2), amount)]


def routed_block(key, own, number, rows, number_of, top, bound, skew):
    order = jax.random.permutation(key, number_of)
    heavy_load, usual = portions_of(number_of, rows * top, bound, skew, True), portions_of(number_of, rows * top, bound, skew, False)
    places = jnp.arange(number_of)

    def named(sizes, offset_by):
        used = int((sizes > 0).sum())
        fixed = max(1, used // 4)
        moved = fixed + (places - fixed + offset_by * (used - fixed)) % max(1, number_of - fixed)
        return jnp.zeros((number_of,), jnp.int32).at[order[jnp.where(places < fixed, places, moved)]].set(jnp.asarray(sizes, jnp.int32))

    sizes = jnp.where(number % 4 == 0, named(heavy_load, number // 4), named(usual, number - number // 4 - 1))
    mixed = jax.random.permutation(jax.random.fold_in(own, 3), number_of)
    giver, receiver = mixed[0:number_of // 2 * 2:2], mixed[1:number_of // 2 * 2:2]
    slack = jnp.minimum(sizes[giver] - 1, bound - sizes[receiver]) // 2
    slack = jnp.where((giver == order[0]) | (receiver == order[0]) | (sizes[receiver] == 0), 0, jnp.maximum(slack, 0))
    moved = jax.random.randint(jax.random.fold_in(own, 4), (number_of // 2,), 0, 1 << 20) % (slack + 1)
    sizes = sizes.at[giver].add(-moved).at[receiver].add(moved)
    members = jnp.searchsorted(jnp.cumsum(sizes), jnp.arange(rows * top), side="right").astype(jnp.int32)
    table = members.reshape(top, rows).T
    table = table[jax.random.permutation(jax.random.fold_in(own, 1), rows)]
    offset_by = jax.random.randint(jax.random.fold_in(own, 2), (rows, 1), 0, top)
    return jnp.take_along_axis(table, (jnp.arange(top)[None, :] + offset_by) % top, axis=1)


def portions_of(amount, total, limit, lean, full):
    loads = [(1 << 20) // math.isqrt(rank ** lean) + 1 for rank in range(1, amount + 1)]
    largest = limit if full else min(limit, max(-(-total // amount), total * loads[0] // sum(loads)))
    least = 1 if total - largest >= amount - 1 else 0
    counts, surplus = [largest] + [least] * (amount - 1), total - largest - least * (amount - 1)
    while surplus > 0:
        candidates = [i for i in range(1, amount) if counts[i] < largest] or [i for i in range(1, amount) if counts[i] < limit]
        pool, left = sum([loads[i] for i in candidates]), surplus
        for i in candidates:
            addition = min(limit - counts[i], max(1, left * loads[i] // pool), surplus)
            counts[i] = counts[i] + addition
            surplus = surplus - addition
    return np.array(counts)


def centred(key, shape, deviation, most, shards=(), kind=jnp.bfloat16):
    array = jax.random.normal(key, shape, jnp.float32) * deviation
    if len(shards) > 0:
        array = levels(key, shape, shards, -0.22, 0.18) * array
    return jnp.clip(array, min=-most, max=most).astype(kind)


def setup_inputs(seed: int = 0, part: int = 0) -> dict:
    streams_of = jax.random.split(jax.random.key(seed), 10)
    part_keys = jax.random.split(jax.random.fold_in(streams_of[9], part), 10)
    tokens = centred(part_keys[0], (SLOTS, D), 1.0, 6.0, ((0, 16),))
    lengths = uneven(part_keys[1], SEQS, 3 * SEQS, SPAN, 2).astype(jnp.int32)
    experts_keys = jax.random.split(jax.random.fold_in(part_keys[2], 1), SLOTS // SLOTS_DEV)
    experts_turns = jax.random.permutation(jax.random.fold_in(part_keys[2], 3), SLOTS // SLOTS_DEV)
    experts = jax.vmap(lambda own, number: routed_block(jax.random.fold_in(part_keys[2], 2), own, number, SLOTS_DEV, EXPERTS, TOP, CAP, 2))(experts_keys, experts_turns).reshape((SLOTS, TOP))
    route_weights = jnp.clip(0.2 + 0.8 * jax.random.uniform(part_keys[3], (SLOTS, TOP), jnp.float32) ** levels(part_keys[3], (SLOTS, TOP), ((0, 16),), -0.2, 0.2), 0.2, 1.0)
    gate_proj = centred(streams_of[4], (N_EP, D, FF_DEV), D ** -0.5, 0.125, ((0, 16),))
    up_proj = centred(streams_of[5], (N_EP, D, FF_DEV), D ** -0.5, 0.125, ((0, 16),))
    down_proj = centred(streams_of[6], (N_EP, FF_DEV, D), FF ** -0.5, 0.0625, ((0, 16),))
    norm_gain = jnp.clip(1.0 + 0.18 * jax.random.normal(streams_of[7], (D,), jnp.float32), 0.1, 1.9)
    norm_bias = centred(streams_of[8], (D,), 0.5, 3.0, (), jnp.float32)
    return dict(tokens=tokens, lengths=lengths, experts=experts, route_weights=route_weights, gate_proj=gate_proj, up_proj=up_proj, down_proj=down_proj, norm_gain=norm_gain, norm_bias=norm_bias)


RESIDUAL_SCALE = 8.0 ** 0.25
NORM_EPS = 1e-05

def layer_norm(values, norm_gain, norm_bias):
    center = values - lax.optimization_barrier(jnp.mean(values, -1, keepdims=True))
    variance = lax.optimization_barrier(jnp.mean(center * center, -1, keepdims=True))
    return center * lax.rsqrt(variance + NORM_EPS) * norm_gain.astype(jnp.float32) + norm_bias.astype(jnp.float32)

def reference(tokens, lengths, experts, route_weights, gate_proj, up_proj, down_proj, norm_gain, norm_bias):
    slot_total = tokens.shape[0]
    position = jnp.arange(slot_total, dtype=jnp.int32)
    alive_mask = position % SPAN < jnp.repeat(lengths, SPAN, total_repeat_length=slot_total)
    expert_ids = jnp.arange(EXPERTS, dtype=jnp.int32)
    chosen = experts[:, :, None] == expert_ids[None, None, :]
    mixing = lax.optimization_barrier(jnp.sum(jnp.where(chosen, route_weights[:, :, None], 0.0), axis=1))
    mixing = jnp.where(alive_mask[:, None], mixing, 0.0).astype(jnp.float32)
    inputs = tokens.astype(jnp.float32)
    gate_all = gate_proj.reshape(EXPERTS, SPLIT, D, FF_DEV)
    up_all = up_proj.reshape(EXPERTS, SPLIT, D, FF_DEV)
    down_all = down_proj.reshape(EXPERTS, FF, D)

    def one_expert(running, pieces):
        gate_block, up_block, down_block, weight_col = pieces
        gate_full = gate_block.transpose(1, 0, 2).reshape(D, FF).astype(jnp.float32)
        up_full = up_block.transpose(1, 0, 2).reshape(D, FF).astype(jnp.float32)
        pre_gate = jnp.dot(inputs, gate_full, precision=lax.Precision.HIGHEST)
        pre_up = jnp.dot(inputs, up_full, precision=lax.Precision.HIGHEST)
        hidden = (jax.nn.silu(pre_gate) * pre_up).astype(jnp.bfloat16)
        hidden = lax.optimization_barrier(hidden).astype(jnp.float32)
        result = jnp.dot(hidden, down_block.astype(jnp.float32), precision=lax.Precision.HIGHEST)
        return (running + weight_col[:, None] * result, None)
    running, _ = lax.scan(one_expert, jnp.zeros((slot_total, D), jnp.float32), (gate_all, up_all, down_all, mixing.T))
    normed = layer_norm(RESIDUAL_SCALE * inputs + running, norm_gain, norm_bias)
    return jnp.where(alive_mask[:, None], normed, 0.0).astype(jnp.bfloat16)
```

```python
import functools
import jax
import jax.numpy as jnp
from jax import lax
from jax.experimental import pallas as pl
from jax.experimental.pallas import tpu as pltpu
from jax.sharding import PartitionSpec as P

SPLIT = 4
TOP = 2
SPAN = 8
MEAN_LIVE = 3

RESIDUAL_SCALE = 8.0**0.25
NORM_EPS = 1e-05
MESH = pl.DeviceIdType.MESH
CHUNKS = 2


def ring_chip(place, chips):
    half = chips // 2
    far = place // half
    return (1 - far) * 2 * place + far * (2 * (chips - 1 - place) + 1)


def ring_place(chip, chips):
    depth, side = chip // 2, chip % 2
    return (1 - side) * depth + side * (chips - 1 - depth)


def neighbourhood(devices):
    chips = devices // 2
    me = lax.axis_index("ep")
    core = me % 2
    place = ring_place(me // 2, chips)
    right = ring_chip((place + 1) % chips, chips) * 2 + core
    left = ring_chip((place + chips - 1) % chips, chips) * 2 + core
    mate = me + 1 - 2 * core
    return chips, me, core, place, (right, left), mate


def greet(others):
    barrier = pltpu.get_barrier_semaphore()
    for other in others:
        pl.semaphore_signal(barrier, inc=1, device_id={"ep": other}, device_id_type=MESH)
    pl.semaphore_wait(barrier, len(others))


def gather_kernel(
    devices, x_ref, m_ref, out_ref, meta_ref,
    send, recv, mate_send, mate_recv, msend, mrecv, mmate_send, mmate_recv, own_sem,
):
    chips, me, core, place, sides, mate = neighbourhood(devices)
    rows = x_ref.shape[0]
    part = rows // 2
    piece = part // CHUNKS
    greet((*sides, mate))

    def remote(src, dst, s_sem, r_sem, device):
        return pltpu.make_async_remote_copy(
            src_ref=src, dst_ref=dst, send_sem=s_sem, recv_sem=r_sem,
            device_id={"ep": device}, device_id_type=MESH,
        )

    def block_at(way, step):
        shift = chips - step if way == 0 else step
        return ring_chip((place + shift) % chips, chips) * 2 + core

    def hop(way, k, step, first=False):
        block = block_at(way, step)
        span = pl.ds(way * part + k * piece, piece)
        src = x_ref.at[span] if first else out_ref.at[block, span]
        return remote(
            src, out_ref.at[block, span], send.at[step, way, k], recv.at[step, way, k], sides[way]
        )

    def share(way, step):
        block = block_at(way, step + 1)
        span = pl.ds(way * part, part)
        view = out_ref.at[block, span]
        return remote(view, view, mate_send.at[step, way], mate_recv.at[step, way], mate)

    def meta_hop(step, first=False):
        block = block_at(0, step)
        src = m_ref if first else meta_ref.at[block]
        return remote(src, meta_ref.at[block], msend.at[step], mrecv.at[step], sides[0])

    def meta_share(step):
        view = meta_ref.at[block_at(0, step + 1)]
        return remote(view, view, mmate_send.at[step], mmate_recv.at[step], mate)

    last = chips - 1
    meta_hop(0, True).start()
    for k in range(CHUNKS):
        for way in range(2):
            hop(way, k, 0, True).start()
    own = pltpu.make_async_copy(x_ref, out_ref.at[me], own_sem.at[0])
    own_meta = pltpu.make_async_copy(m_ref, meta_ref.at[me], own_sem.at[1])
    own.start()
    own_meta.start()
    own_share = remote(
        x_ref, out_ref.at[me], mate_send.at[last, 0], mate_recv.at[last, 0], mate
    )
    own_meta_share = remote(
        m_ref, meta_ref.at[me], mmate_send.at[last], mmate_recv.at[last], mate
    )
    own_share.start()
    own_meta_share.start()

    def advance(step, onward):
        meta_hop(step).wait_recv()
        if onward:
            meta_hop(step + 1).start()
        meta_share(step).start()
        for k in range(CHUNKS):
            for way in range(2):
                hop(way, k, step).wait_recv()
                if onward:
                    hop(way, k, step + 1).start()
        for way in range(2):
            share(way, step).start()

    @pl.loop(0, chips - 2)
    def _(step):
        advance(step, True)

    advance(chips - 2, False)

    @pl.loop(0, chips - 1)
    def _(step):
        meta_hop(step).wait_send()
        meta_share(step).wait()
        for way in range(2):
            for k in range(CHUNKS):
                hop(way, k, step).wait_send()
            share(way, step).wait()

    own.wait()
    own_meta.wait()
    own_share.wait()
    own_meta_share.wait()


def gather_all(tokens, meta, devices):
    rows, width = tokens.shape
    chips = devices // 2
    vmem = pl.BlockSpec(memory_space=pltpu.VMEM)
    dma = pltpu.SemaphoreType.DMA
    return pl.pallas_call(
        functools.partial(gather_kernel, devices),
        out_shape=(
            jax.ShapeDtypeStruct((devices, rows, width), tokens.dtype),
            jax.ShapeDtypeStruct((devices, *meta.shape), meta.dtype),
        ),
        in_specs=[vmem, vmem],
        out_specs=(vmem, vmem),
        scratch_shapes=[
            dma((chips - 1, 2, CHUNKS)), dma((chips - 1, 2, CHUNKS)),
            dma((chips, 2)), dma((chips, 2)),
            dma((chips - 1,)), dma((chips - 1,)),
            dma((chips,)), dma((chips,)),
            dma((2,)),
        ],
        compiler_params=pltpu.CompilerParams(collective_id=0, has_side_effects=True),
        name="ring_gather",
    )(tokens, meta)


def scatter_kernel(
    devices, y_ref, spread_ref, tokens_ref, alive_ref, gain_ref, bias_ref, out_ref,
    mate_sum, high, low, stage, inbox, final, landed,
    swap_send, swap_recv, send, recv, final_send, final_recv,
):
    chips, me, core, place, sides, mate = neighbourhood(devices)
    rows, width = tokens_ref.shape
    half = width // 2
    quarter = half // 2
    greet((*sides, mate))
    here = pl.ds(pl.multiple_of(core * half, half), half)
    there = pl.ds(pl.multiple_of((1 - core) * half, half), half)

    def remote(src, dst, s_sem, r_sem, device):
        return pltpu.make_async_remote_copy(
            src_ref=src, dst_ref=dst, send_sem=s_sem, recv_sem=r_sem,
            device_id={"ep": device}, device_id_type=MESH,
        )

    swap = remote(y_ref.at[:, there], mate_sum, swap_send, swap_recv, mate)
    swap.start()
    swap.wait()
    total = y_ref[:, here] + mate_sum[...]
    top = total.astype(jnp.bfloat16)
    high[...] = top
    low[...] = (total - top.astype(jnp.float32)).astype(jnp.bfloat16)

    def local_part(way, k, step):
        shift = chips - 1 - step if way == 0 else 1 + step
        chip = ring_chip((place + shift) % chips, chips)
        start = pl.multiple_of((chip * 2 + k) * rows, rows)
        picks = spread_ref[pl.ds(start, rows), :]
        columns = pl.ds(way * quarter, quarter)
        return jnp.dot(
            picks, high[:, columns], preferred_element_type=jnp.float32
        ) + jnp.dot(picks, low[:, columns], preferred_element_type=jnp.float32)

    def hop(way, k, step):
        return remote(
            stage.at[step, way, k], inbox.at[step, way, k],
            send.at[step, way, k], recv.at[step, way, k], sides[way],
        )

    for k in range(2):
        for way in range(2):
            stage[0, way, k] = local_part(way, k, 0).astype(jnp.bfloat16)
            hop(way, k, 0).start()

    @pl.loop(1, chips - 1)
    def _(step):
        for k in range(2):
            for way in range(2):
                mine = local_part(way, k, step)
                hop(way, k, step - 1).wait_recv()
                stage[step, way, k] = (
                    mine + inbox[step - 1, way, k].astype(jnp.float32)
                ).astype(jnp.bfloat16)
                hop(way, k, step).start()

    for k in range(2):
        for way in range(2):
            mine = local_part(way, k, chips - 1)
            hop(way, k, chips - 2).wait_recv()
            final[k, :, way * quarter:(way + 1) * quarter] = (
                mine + inbox[chips - 2, way, k].astype(jnp.float32)
            )
    give = remote(final.at[1 - core], landed, final_send, final_recv, mate)
    give.start()

    @pl.loop(0, chips - 1)
    def _(step):
        for k in range(2):
            for way in range(2):
                hop(way, k, step).wait_send()

    give.wait()
    ours = final[core]
    theirs = landed[...]
    first = core == 0
    branch = jnp.concatenate(
        [jnp.where(first, ours, theirs), jnp.where(first, theirs, ours)], axis=1
    )
    values = RESIDUAL_SCALE * tokens_ref[...].astype(jnp.float32) + branch
    center = values - jnp.mean(values, -1, keepdims=True)
    variance = jnp.mean(center * center, -1, keepdims=True)
    normed = center * lax.rsqrt(variance + NORM_EPS) * gain_ref[...] + bias_ref[...]
    out_ref[...] = jnp.where(alive_ref[...] > 0, normed, 0.0).astype(jnp.bfloat16)


def scatter_norm(y, spread, tokens, alive, gain, bias, devices):
    rows, width = tokens.shape
    live = y.shape[0]
    chips = devices // 2
    half, quarter = width // 2, width // 4
    vmem = pl.BlockSpec(memory_space=pltpu.VMEM)
    dma = pltpu.SemaphoreType.DMA
    return pl.pallas_call(
        functools.partial(scatter_kernel, devices),
        out_shape=jax.ShapeDtypeStruct((rows, width), jnp.bfloat16),
        in_specs=[vmem] * 6,
        out_specs=vmem,
        scratch_shapes=[
            pltpu.VMEM((live, half), jnp.float32),
            pltpu.VMEM((live, half), jnp.bfloat16),
            pltpu.VMEM((live, half), jnp.bfloat16),
            pltpu.VMEM((chips - 1, 2, 2, rows, quarter), jnp.bfloat16),
            pltpu.VMEM((chips - 1, 2, 2, rows, quarter), jnp.bfloat16),
            pltpu.VMEM((2, rows, half), jnp.float32),
            pltpu.VMEM((rows, half), jnp.float32),
            dma, dma,
            dma((chips - 1, 2, 2)), dma((chips - 1, 2, 2)),
            dma, dma,
        ],
        compiler_params=pltpu.CompilerParams(
            collective_id=1, has_side_effects=True, vmem_limit_bytes=48 * 1024 * 1024
        ),
        name="ring_scatter_norm",
    )(y, spread, tokens, alive, gain, bias)


def local(
    tokens, lengths, experts, route_weights, gate_proj, up_proj, down_proj, norm_gain, norm_bias
):
    rows, width = tokens.shape
    devices = lax.axis_size("ep")
    expert_count = devices // SPLIT
    seqs = lengths.shape[0]
    live = MEAN_LIVE * seqs * devices
    alive = (jnp.arange(SPAN, dtype=jnp.int32)[None, :] < lengths[:, None]).reshape(rows)
    meta_rows = -(-(expert_count + 1) // 8) * 8
    ids = jnp.arange(meta_rows, dtype=jnp.int32)
    named = experts.T[None, :, :] == ids[:, None, None]
    mixing = jnp.sum(jnp.where(named, route_weights.T[None, :, :], 0.0), axis=1)
    mixing = jnp.where(ids[:, None] == expert_count, 1.0, mixing)
    meta = jnp.where(alive[None, :], mixing, 0.0)
    meta = jnp.pad(meta, ((0, 0), (0, -rows % 128)))
    gathered, metas = gather_all(tokens, meta, devices)
    gathered = gathered.reshape(devices * rows, width)
    own_expert = lax.axis_index("ep") // SPLIT
    weights = lax.dynamic_index_in_dim(metas, own_expert, 1, keepdims=False)[:, :rows]
    living = metas[:, expert_count, :rows]
    upto = jnp.arange(rows)[:, None] <= jnp.arange(rows)[None, :]
    within = jnp.dot(
        living.astype(jnp.bfloat16), upto.astype(jnp.bfloat16),
        preferred_element_type=jnp.float32,
    )
    counts = within[:, -1]
    before = jnp.sum(
        jnp.where(jnp.arange(devices)[:, None] > jnp.arange(devices)[None, :], counts[None, :], 0.0),
        axis=1,
    )
    rank = (within + before[:, None] - 1.0).astype(jnp.int32)
    rank = jnp.where(living > 0, rank, -1).reshape(devices * rows)
    places = jnp.arange(live, dtype=jnp.int32)
    match = rank[None, :] == places[:, None]
    weight = jnp.sum(jnp.where(match, weights.reshape(-1)[None, :], 0.0), axis=1)
    picked = jnp.dot(
        match.astype(jnp.bfloat16), gathered, preferred_element_type=jnp.float32
    ).astype(jnp.bfloat16)
    pre_gate = jnp.dot(picked, gate_proj[0], preferred_element_type=jnp.float32)
    pre_up = jnp.dot(picked, up_proj[0], preferred_element_type=jnp.float32)
    hidden = (jax.nn.silu(pre_gate) * pre_up).astype(jnp.bfloat16)
    y = jnp.dot(hidden, down_proj[0], preferred_element_type=jnp.float32) * weight[:, None]
    spread = (rank[:, None] == places[None, :]).astype(jnp.bfloat16)
    return scatter_norm(
        y, spread, tokens, alive.astype(jnp.float32)[:, None],
        norm_gain[None, :], norm_bias[None, :], devices,
    )


def solution(mesh):
    in_specs = (
        P(("grp", "ep"), None),
        P(("grp", "ep")),
        P(("grp", "ep"), None),
        P(("grp", "ep"), None),
        P("ep", None, None),
        P("ep", None, None),
        P("ep", None, None),
        P(),
        P(),
    )
    out_specs = P(("grp", "ep"), None)
    return jax.shard_map(local, mesh=mesh, in_specs=in_specs, out_specs=out_specs, check_vma=False)
```

```python
import functools
import jax
import jax.numpy as jnp
from jax import lax
from jax.experimental import pallas as pl
from jax.experimental.pallas import tpu as pltpu
from jax.sharding import PartitionSpec as P

SPLIT = 4
TOP = 2
SPAN = 8
MEAN_LIVE = 3

RESIDUAL_SCALE = 8.0**0.25
NORM_EPS = 1e-05
MESH = pl.DeviceIdType.MESH
CHUNKS = 4


def ring_chip(place, chips):
    half = chips // 2
    far = place // half
    return (1 - far) * 2 * place + far * (2 * (chips - 1 - place) + 1)


def ring_place(chip, chips):
    depth, side = chip // 2, chip % 2
    return (1 - side) * depth + side * (chips - 1 - depth)


def neighbourhood(devices):
    chips = devices // 2
    me = lax.axis_index("ep")
    core = me % 2
    place = ring_place(me // 2, chips)
    right = ring_chip((place + 1) % chips, chips) * 2 + core
    left = ring_chip((place + chips - 1) % chips, chips) * 2 + core
    mate = me + 1 - 2 * core
    return chips, me, core, place, (right, left), mate


def greet(others):
    barrier = pltpu.get_barrier_semaphore()
    for other in others:
        pl.semaphore_signal(barrier, inc=1, device_id={"ep": other}, device_id_type=MESH)
    pl.semaphore_wait(barrier, len(others))


def remote(src, dst, s_sem, r_sem, device):
    return pltpu.make_async_remote_copy(
        src_ref=src, dst_ref=dst, send_sem=s_sem, recv_sem=r_sem,
        device_id={"ep": device}, device_id_type=MESH,
    )


def layer_kernel(
    devices, expert_count,
    x_ref, m_ref, gate_hbm, up_hbm, down_hbm, alive_ref, gain_ref, bias_ref, out_ref,
    all_x, all_meta, gate_ref, up_ref, down_ref,
    chip_meta, living, match_ref, spread_ref, picked, hidden, mate_give, mate_sum, mine_y,
    stage, inbox, final, landed,
    weight_sem, send, recv, mate_send, mate_recv, msend, mrecv, mmate_send, mmate_recv, own_sem,
    swap_send, swap_recv, rsend, rrecv, final_send, final_recv,
):
    chips, me, core, place, sides, mate = neighbourhood(devices)
    rows, width = x_ref.shape
    live = picked.shape[0]
    hidden_units = hidden.shape[1]
    part = rows // 2
    piece = width // CHUNKS
    half = width // 2
    quarter = half // 2
    loads = [
        pltpu.make_async_copy(gate_hbm.at[0], gate_ref, weight_sem.at[0]),
        pltpu.make_async_copy(up_hbm.at[0], up_ref, weight_sem.at[1]),
        pltpu.make_async_copy(down_hbm.at[0], down_ref, weight_sem.at[2]),
    ]
    greet((*sides, mate))

    def block_at(way, step):
        shift = chips - step if way == 0 else step
        return ring_chip((place + shift) % chips, chips) * 2 + core

    def hop(way, k, step, first=False):
        block = block_at(way, step)
        span, columns = pl.ds(way * part, part), pl.ds(k * piece, piece)
        src = x_ref.at[span, columns] if first else all_x.at[block, span, columns]
        return remote(
            src, all_x.at[block, span, columns],
            send.at[step, way, k], recv.at[step, way, k], sides[way],
        )

    def share(way, step):
        view = all_x.at[block_at(way, step + 1), pl.ds(way * part, part)]
        return remote(view, view, mate_send.at[step, way], mate_recv.at[step, way], mate)

    def meta_hop(step, first=False):
        block = block_at(0, step)
        src = m_ref if first else all_meta.at[block]
        return remote(src, all_meta.at[block], msend.at[step], mrecv.at[step], sides[0])

    def meta_share(step):
        view = all_meta.at[block_at(0, step + 1)]
        return remote(view, view, mmate_send.at[step], mmate_recv.at[step], mate)

    last = chips - 1
    meta_hop(0, True).start()
    for k in range(CHUNKS):
        for way in range(2):
            hop(way, k, 0, True).start()
    own = pltpu.make_async_copy(x_ref, all_x.at[me], own_sem.at[0])
    own_meta = pltpu.make_async_copy(m_ref, all_meta.at[me], own_sem.at[1])
    own.start()
    own_meta.start()
    own_share = remote(x_ref, all_x.at[me], mate_send.at[last, 0], mate_recv.at[last, 0], mate)
    own_meta_share = remote(
        m_ref, all_meta.at[me], mmate_send.at[last], mmate_recv.at[last], mate
    )
    own_share.start()
    own_meta_share.start()
    for load in loads:
        load.start()

    def advance(step, onward):
        meta_hop(step).wait_recv()
        if onward:
            meta_hop(step + 1).start()
        meta_share(step).start()
        for k in range(CHUNKS):
            for way in range(2):
                hop(way, k, step).wait_recv()
                if onward:
                    hop(way, k, step + 1).start()
        for way in range(2):
            share(way, step).start()

    @pl.loop(0, chips - 2)
    def _(step):
        advance(step, True)

    advance(chips - 2, False)

    @pl.loop(0, chips - 1)
    def _(step):
        meta_hop(step).wait_send()
        meta_share(step).wait()
        for way in range(2):
            for k in range(CHUNKS):
                hop(way, k, step).wait_send()
            share(way, step).wait()

    own.wait()
    own_meta.wait()
    own_share.wait()
    own_meta_share.wait()

    lanes = 2 * rows
    for q in range(chips):
        pair = all_meta[2 * q] + all_meta[2 * q + 1]
        chip_meta[q] = pair
        living[q:q + 1, :] = pair[expert_count:expert_count + 1, :]
    lives = living[...]
    upto = (
        lax.broadcasted_iota(jnp.int32, (lanes, lanes), 0)
        <= lax.broadcasted_iota(jnp.int32, (lanes, lanes), 1)
    )
    within = jnp.dot(lives, upto.astype(jnp.float32), preferred_element_type=jnp.float32)
    own_expert = me // SPLIT
    line = lax.broadcasted_iota(jnp.int32, (live, lanes), 0).astype(jnp.float32)
    weight_sum = jnp.zeros((live, lanes), jnp.float32)
    before = jnp.full((1, 1), -1.0, jnp.float32)
    for q in range(chips):
        lived = lives[q:q + 1, :]
        rank = jnp.where(lived > 0, within[q:q + 1, :] + before, -1.0)
        before = before + jnp.sum(lived, 1, keepdims=True)
        same = line == rank
        weight_sum += jnp.where(same, chip_meta[q, pl.ds(own_expert, 1), :], 0.0)
        ones = same.astype(jnp.float32)
        match_ref[:, q * lanes:(q + 1) * lanes] = ones.astype(jnp.bfloat16)
        spread_ref[q * lanes:(q + 1) * lanes, :] = jnp.transpose(ones).astype(jnp.bfloat16)
    weight = jnp.sum(weight_sum, 1, keepdims=True)

    tile = 256

    @pl.loop(0, width // tile)
    def _(t):
        columns = pl.ds(pl.multiple_of(t * tile, tile), tile)
        rows_all = all_x[:, :, columns].reshape(devices * rows, tile)
        picked[:, columns] = jnp.dot(
            match_ref[...], rows_all, preferred_element_type=jnp.float32
        ).astype(jnp.bfloat16)

    for load in loads[:2]:
        load.wait()

    @pl.loop(0, hidden_units // tile)
    def _(t):
        columns = pl.ds(pl.multiple_of(t * tile, tile), tile)
        g = jnp.dot(picked[...], gate_ref[:, columns], preferred_element_type=jnp.float32)
        u = jnp.dot(picked[...], up_ref[:, columns], preferred_element_type=jnp.float32)
        hidden[:, columns] = (jax.nn.silu(g) * u).astype(jnp.bfloat16)

    loads[2].wait()

    def down_into(base, dst):
        @pl.loop(0, half // tile)
        def _(t):
            columns = pl.ds(pl.multiple_of(t * tile, tile), tile)
            source = pl.ds(pl.multiple_of(base + t * tile, tile), tile)
            dst[:, columns] = weight * jnp.dot(
                hidden[...], down_ref[:, source], preferred_element_type=jnp.float32
            )

    down_into((1 - core) * half, mate_give)
    swap = remote(mate_give, mate_sum, swap_send, swap_recv, mate)
    swap.start()
    down_into(core * half, mine_y)
    swap.wait()
    total = mine_y[...] + mate_sum[...]
    top = total.astype(jnp.bfloat16)
    high, low = picked.at[:, pl.ds(0, half)], picked.at[:, pl.ds(half, half)]
    high[...] = top
    low[...] = (total - top.astype(jnp.float32)).astype(jnp.bfloat16)

    cut = lanes // CHUNKS

    def local_part(way, step):
        shift = chips - 1 - step if way == 0 else 1 + step
        chip = ring_chip((place + shift) % chips, chips)
        picks = spread_ref[pl.ds(pl.multiple_of(chip * lanes, lanes), lanes), :]
        columns = pl.ds(way * quarter, quarter)
        return jnp.dot(
            picks, high[:, columns], preferred_element_type=jnp.float32
        ) + jnp.dot(picks, low[:, columns], preferred_element_type=jnp.float32)

    def pass_on(way, k, step):
        return remote(
            stage.at[step, way, k], inbox.at[step, way, k],
            rsend.at[step, way, k], rrecv.at[step, way, k], sides[way],
        )

    for way in range(2):
        part_sum = local_part(way, 0)
        for k in range(CHUNKS):
            stage[0, way, k] = part_sum[k * cut:(k + 1) * cut].astype(jnp.bfloat16)
            pass_on(way, k, 0).start()

    @pl.loop(1, chips - 1)
    def _(step):
        sums = [local_part(way, step) for way in range(2)]
        for k in range(CHUNKS):
            for way in range(2):
                pass_on(way, k, step - 1).wait_recv()
                stage[step, way, k] = (
                    sums[way][k * cut:(k + 1) * cut]
                    + inbox[step - 1, way, k].astype(jnp.float32)
                ).astype(jnp.bfloat16)
                pass_on(way, k, step).start()

    sums = [local_part(way, chips - 1) for way in range(2)]
    for k in range(CHUNKS):
        for way in range(2):
            pass_on(way, k, chips - 2).wait_recv()
            final[k * cut:(k + 1) * cut, way * quarter:(way + 1) * quarter] = (
                sums[way][k * cut:(k + 1) * cut]
                + inbox[chips - 2, way, k].astype(jnp.float32)
            )
    theirs_at = pl.ds(pl.multiple_of((1 - core) * rows, rows), rows)
    ours_at = pl.ds(pl.multiple_of(core * rows, rows), rows)
    give = remote(final.at[theirs_at], landed, final_send, final_recv, mate)
    give.start()

    @pl.loop(0, chips - 1)
    def _(step):
        for k in range(CHUNKS):
            for way in range(2):
                pass_on(way, k, step).wait_send()

    give.wait()
    ours = final[ours_at, :]
    theirs = landed[...]
    first = core == 0
    branch = jnp.concatenate(
        [jnp.where(first, ours, theirs), jnp.where(first, theirs, ours)], axis=1
    )
    values = RESIDUAL_SCALE * x_ref[...].astype(jnp.float32) + branch
    center = values - jnp.mean(values, -1, keepdims=True)
    variance = jnp.mean(center * center, -1, keepdims=True)
    normed = center * lax.rsqrt(variance + NORM_EPS) * gain_ref[...] + bias_ref[...]
    out_ref[...] = jnp.where(alive_ref[...] > 0, normed, 0.0).astype(jnp.bfloat16)


def whole_layer(tokens, meta, gate, up, down, alive, gain, bias, devices, expert_count, live):
    rows, width = tokens.shape
    chips = devices // 2
    units = gate.shape[2]
    half, quarter = width // 2, width // 4
    vmem = pl.BlockSpec(memory_space=pltpu.VMEM)
    anywhere = pl.BlockSpec(memory_space=pl.ANY)
    dma = pltpu.SemaphoreType.DMA
    bf16, f32 = jnp.bfloat16, jnp.float32
    ring = (chips - 1, 2, CHUNKS)
    return pl.pallas_call(
        functools.partial(layer_kernel, devices, expert_count),
        out_shape=jax.ShapeDtypeStruct((rows, width), bf16),
        in_specs=[vmem, vmem, anywhere, anywhere, anywhere, vmem, vmem, vmem],
        out_specs=vmem,
        scratch_shapes=[
            pltpu.VMEM((devices, rows, width), bf16),
            pltpu.VMEM((devices, *meta.shape), f32),
            pltpu.VMEM(gate.shape[1:], bf16),
            pltpu.VMEM(up.shape[1:], bf16),
            pltpu.VMEM(down.shape[1:], bf16),
            pltpu.VMEM((chips, *meta.shape), f32),
            pltpu.VMEM((chips, 2 * rows), f32),
            pltpu.VMEM((live, devices * rows), bf16),
            pltpu.VMEM((devices * rows, live), bf16),
            pltpu.VMEM((live, width), bf16),
            pltpu.VMEM((live, units), bf16),
            pltpu.VMEM((live, half), f32),
            pltpu.VMEM((live, half), f32),
            pltpu.VMEM((live, half), f32),
            pltpu.VMEM((*ring, 2 * rows // CHUNKS, quarter), bf16),
            pltpu.VMEM((*ring, 2 * rows // CHUNKS, quarter), bf16),
            pltpu.VMEM((2 * rows, half), f32),
            pltpu.VMEM((rows, half), f32),
            dma((3,)),
            dma(ring), dma(ring),
            dma((chips, 2)), dma((chips, 2)),
            dma((chips - 1,)), dma((chips - 1,)),
            dma((chips,)), dma((chips,)),
            dma((2,)),
            dma, dma,
            dma(ring), dma(ring),
            dma, dma,
        ],
        compiler_params=pltpu.CompilerParams(
            collective_id=0, has_side_effects=True, vmem_limit_bytes=67043328
        ),
        name="layer",
    )(tokens, meta, gate, up, down, alive, gain, bias)


def local(
    tokens, lengths, experts, route_weights, gate_proj, up_proj, down_proj, norm_gain, norm_bias
):
    rows, width = tokens.shape
    devices = lax.axis_size("ep")
    expert_count = devices // SPLIT
    seqs = lengths.shape[0]
    live = MEAN_LIVE * seqs * devices
    alive = (jnp.arange(SPAN, dtype=jnp.int32)[None, :] < lengths[:, None]).reshape(rows)
    meta_rows = -(-(expert_count + 1) // 8) * 8
    ids = jnp.arange(meta_rows, dtype=jnp.int32)
    named = experts.T[None, :, :] == ids[:, None, None]
    mixing = jnp.sum(jnp.where(named, route_weights.T[None, :, :], 0.0), axis=1)
    mixing = jnp.where(ids[:, None] == expert_count, 1.0, mixing)
    meta = jnp.where(alive[None, :], mixing, 0.0)
    core = lax.axis_index("ep") % 2
    blank = jnp.zeros_like(meta)
    meta = jnp.where(
        core == 0,
        jnp.concatenate([meta, blank], axis=1),
        jnp.concatenate([blank, meta], axis=1),
    )
    return whole_layer(
        tokens, meta, gate_proj, up_proj, down_proj, alive.astype(jnp.float32)[:, None],
        norm_gain[None, :], norm_bias[None, :], devices, expert_count, live,
    )


def solution(mesh):
    in_specs = (
        P(("grp", "ep"), None),
        P(("grp", "ep")),
        P(("grp", "ep"), None),
        P(("grp", "ep"), None),
        P("ep", None, None),
        P("ep", None, None),
        P("ep", None, None),
        P(),
        P(),
    )
    out_specs = P(("grp", "ep"), None)
    return jax.shard_map(local, mesh=mesh, in_specs=in_specs, out_specs=out_specs, check_vma=False)
```

```python
import functools
import jax
import jax.numpy as jnp
from jax import lax
from jax.experimental import pallas as pl
from jax.experimental.pallas import tpu as pltpu
from jax.sharding import PartitionSpec as P

SPLIT = 4
TOP = 2
SPAN = 8
MEAN_LIVE = 3

RESIDUAL_SCALE = 8.0**0.25
NORM_EPS = 1e-05
MESH = pl.DeviceIdType.MESH
CHUNKS = 4


def ring_chip(place, chips):
    half = chips // 2
    far = place // half
    return (1 - far) * 2 * place + far * (2 * (chips - 1 - place) + 1)


def ring_place(chip, chips):
    depth, side = chip // 2, chip % 2
    return (1 - side) * depth + side * (chips - 1 - depth)


def neighbourhood(devices):
    chips = devices // 2
    me = lax.axis_index("ep")
    core = me % 2
    place = ring_place(me // 2, chips)
    right = ring_chip((place + 1) % chips, chips) * 2 + core
    left = ring_chip((place + chips - 1) % chips, chips) * 2 + core
    mate = me + 1 - 2 * core
    return chips, me, core, place, (right, left), mate


def greet(others):
    barrier = pltpu.get_barrier_semaphore()
    for other in others:
        pl.semaphore_signal(barrier, inc=1, device_id={"ep": other}, device_id_type=MESH)
    pl.semaphore_wait(barrier, len(others))


def remote(src, dst, s_sem, r_sem, device):
    return pltpu.make_async_remote_copy(
        src_ref=src, dst_ref=dst, send_sem=s_sem, recv_sem=r_sem,
        device_id={"ep": device}, device_id_type=MESH,
    )


def layer_kernel(
    devices, expert_count,
    x_ref, m_ref, gate_hbm, up_hbm, down_hbm, lengths_ref, gain_ref, bias_ref, out_ref,
    all_x, all_meta, gate_ref, up_ref, down_ref,
    chip_meta, living, match_ref, spread_ref, picked, hidden, mate_give, mate_sum, mine_y,
    stage, inbox, final, landed,
    weight_sem, send, recv, mate_send, mate_recv, msend, mrecv, mmate_send, mmate_recv, own_sem,
    swap_send, swap_recv, rsend, rrecv, final_send, final_recv,
):
    chips, me, core, place, sides, mate = neighbourhood(devices)
    rows, width = x_ref.shape
    live = picked.shape[0]
    hidden_units = hidden.shape[1]
    part = rows // 2
    piece = width // CHUNKS
    half = width // 2
    quarter = half // 2
    loads = [
        pltpu.make_async_copy(gate_hbm.at[0], gate_ref, weight_sem.at[0]),
        pltpu.make_async_copy(up_hbm.at[0], up_ref, weight_sem.at[1]),
        pltpu.make_async_copy(down_hbm.at[0], down_ref, weight_sem.at[2]),
    ]
    greet((*sides, mate))

    def block_at(way, step):
        shift = chips - step if way == 0 else step
        return ring_chip((place + shift) % chips, chips) * 2 + core

    def hop(way, k, step, first=False):
        block = block_at(way, step)
        span, columns = pl.ds(way * part, part), pl.ds(k * piece, piece)
        src = x_ref.at[span, columns] if first else all_x.at[block, span, columns]
        return remote(
            src, all_x.at[block, span, columns],
            send.at[step, way, k], recv.at[step, way, k], sides[way],
        )

    def share(way, step):
        view = all_x.at[block_at(way, step + 1), pl.ds(way * part, part)]
        return remote(view, view, mate_send.at[step, way], mate_recv.at[step, way], mate)

    def meta_hop(step, first=False):
        block = block_at(0, step)
        src = m_ref if first else all_meta.at[block]
        return remote(src, all_meta.at[block], msend.at[step], mrecv.at[step], sides[0])

    def meta_share(step):
        view = all_meta.at[block_at(0, step + 1)]
        return remote(view, view, mmate_send.at[step], mmate_recv.at[step], mate)

    last = chips - 1
    meta_hop(0, True).start()
    for k in range(CHUNKS):
        for way in range(2):
            hop(way, k, 0, True).start()
    own = pltpu.make_async_copy(x_ref, all_x.at[me], own_sem.at[0])
    own_meta = pltpu.make_async_copy(m_ref, all_meta.at[me], own_sem.at[1])
    own.start()
    own_meta.start()
    own_share = remote(x_ref, all_x.at[me], mate_send.at[last, 0], mate_recv.at[last, 0], mate)
    own_meta_share = remote(
        m_ref, all_meta.at[me], mmate_send.at[last], mmate_recv.at[last], mate
    )
    own_share.start()
    own_meta_share.start()
    for load in loads:
        load.start()

    def advance(step, onward):
        meta_hop(step).wait_recv()
        if onward:
            meta_hop(step + 1).start()
        meta_share(step).start()
        for k in range(CHUNKS):
            for way in range(2):
                hop(way, k, step).wait_recv()
                if onward:
                    hop(way, k, step + 1).start()
        for way in range(2):
            share(way, step).start()

    @pl.loop(0, chips - 2)
    def _(step):
        advance(step, True)

    advance(chips - 2, False)

    @pl.loop(0, chips - 1)
    def _(step):
        meta_hop(step).wait_send()
        meta_share(step).wait()
        for way in range(2):
            for k in range(CHUNKS):
                hop(way, k, step).wait_send()
            share(way, step).wait()

    own.wait()
    own_meta.wait()
    own_share.wait()
    own_meta_share.wait()

    lanes = 2 * rows
    for q in range(chips):
        pair = all_meta[2 * q] + all_meta[2 * q + 1]
        chip_meta[q] = pair
        living[q:q + 1, :] = pair[expert_count:expert_count + 1, :]
    lives = living[...]
    upto = (
        lax.broadcasted_iota(jnp.int32, (lanes, lanes), 0)
        <= lax.broadcasted_iota(jnp.int32, (lanes, lanes), 1)
    )
    within = jnp.dot(lives, upto.astype(jnp.float32), preferred_element_type=jnp.float32)
    own_expert = me // SPLIT
    line = lax.broadcasted_iota(jnp.int32, (live, lanes), 0).astype(jnp.float32)
    weight_sum = jnp.zeros((live, lanes), jnp.float32)
    before = jnp.full((1, 1), -1.0, jnp.float32)
    for q in range(chips):
        lived = lives[q:q + 1, :]
        rank = jnp.where(lived > 0, within[q:q + 1, :] + before, -1.0)
        before = before + jnp.sum(lived, 1, keepdims=True)
        same = line == rank
        weight_sum += jnp.where(same, chip_meta[q, pl.ds(own_expert, 1), :], 0.0)
        ones = same.astype(jnp.float32)
        match_ref[:, q * lanes:(q + 1) * lanes] = ones.astype(jnp.bfloat16)
        spread_ref[q * lanes:(q + 1) * lanes, :] = jnp.transpose(ones).astype(jnp.bfloat16)
    weight = jnp.sum(weight_sum, 1, keepdims=True)

    tile = 2 * 256
    slab = hidden_units // 2 if hidden_units % 256 == 0 and devices <= 4 * SPLIT else 256
    slabs = hidden_units // slab

    @pl.loop(0, width // tile)
    def _(t):
        columns = pl.ds(pl.multiple_of(t * tile, tile), tile)
        rows_all = all_x[:, :, columns].reshape(devices * rows, tile)
        picked[:, columns] = jnp.dot(
            match_ref[...], rows_all, preferred_element_type=jnp.float32
        ).astype(jnp.bfloat16)

    for load in loads[:2]:
        load.wait()

    @pl.loop(0, slabs)
    def _(t):
        columns = pl.ds(pl.multiple_of(t * slab, slab), slab)
        g = jnp.dot(picked[...], gate_ref[:, columns], preferred_element_type=jnp.float32)
        u = jnp.dot(picked[...], up_ref[:, columns], preferred_element_type=jnp.float32)
        hidden[:, columns] = (jax.nn.silu(g) * u).astype(jnp.bfloat16)

    loads[2].wait()

    def down_into(base, dst):
        @pl.loop(0, half // tile)
        def _(t):
            columns = pl.ds(pl.multiple_of(t * tile, tile), tile)
            source = pl.ds(pl.multiple_of(base + t * tile, tile), tile)
            dst[:, columns] = weight * jnp.dot(
                hidden[...], down_ref[:, source], preferred_element_type=jnp.float32
            )

    down_into((1 - core) * half, mate_give)
    swap = remote(mate_give, mate_sum, swap_send, swap_recv, mate)
    swap.start()
    down_into(core * half, mine_y)
    swap.wait()
    total = mine_y[...] + mate_sum[...]
    top = total.astype(jnp.bfloat16)
    high, low = picked.at[:, pl.ds(0, half)], picked.at[:, pl.ds(half, half)]
    high[...] = top
    low[...] = (total - top.astype(jnp.float32)).astype(jnp.bfloat16)

    cut = lanes // CHUNKS

    def local_part(way, step):
        shift = chips - 1 - step if way == 0 else 1 + step
        chip = ring_chip((place + shift) % chips, chips)
        picks = spread_ref[pl.ds(pl.multiple_of(chip * lanes, lanes), lanes), :]
        columns = pl.ds(way * quarter, quarter)
        return jnp.dot(
            picks, high[:, columns], preferred_element_type=jnp.float32
        ) + jnp.dot(picks, low[:, columns], preferred_element_type=jnp.float32)

    def pass_on(way, k, step):
        return remote(
            stage.at[step, way, k], inbox.at[step, way, k],
            rsend.at[step, way, k], rrecv.at[step, way, k], sides[way],
        )

    for way in range(2):
        part_sum = local_part(way, 0)
        for k in range(CHUNKS):
            stage[0, way, k] = part_sum[k * cut:(k + 1) * cut].astype(jnp.bfloat16)
            pass_on(way, k, 0).start()

    @pl.loop(1, chips - 1)
    def _(step):
        sums = [local_part(way, step) for way in range(2)]
        for k in range(CHUNKS):
            for way in range(2):
                pass_on(way, k, step - 1).wait_recv()
                stage[step, way, k] = (
                    sums[way][k * cut:(k + 1) * cut]
                    + inbox[step - 1, way, k].astype(jnp.float32)
                ).astype(jnp.bfloat16)
                pass_on(way, k, step).start()

    sums = [local_part(way, chips - 1) for way in range(2)]
    for k in range(CHUNKS):
        for way in range(2):
            pass_on(way, k, chips - 2).wait_recv()
            final[k * cut:(k + 1) * cut, way * quarter:(way + 1) * quarter] = (
                sums[way][k * cut:(k + 1) * cut]
                + inbox[chips - 2, way, k].astype(jnp.float32)
            )
    theirs_at = pl.ds(pl.multiple_of((1 - core) * rows, rows), rows)
    ours_at = pl.ds(pl.multiple_of(core * rows, rows), rows)
    give = remote(final.at[theirs_at], landed, final_send, final_recv, mate)
    give.start()

    @pl.loop(0, chips - 1)
    def _(step):
        for k in range(CHUNKS):
            for way in range(2):
                pass_on(way, k, step).wait_send()

    give.wait()
    ours = final[ours_at, :]
    theirs = landed[...]
    first = core == 0
    branch = jnp.concatenate(
        [jnp.where(first, ours, theirs), jnp.where(first, theirs, ours)], axis=1
    )
    values = RESIDUAL_SCALE * x_ref[...].astype(jnp.float32) + branch
    center = values - jnp.mean(values, -1, keepdims=True)
    variance = jnp.mean(center * center, -1, keepdims=True)
    normed = center * lax.rsqrt(variance + NORM_EPS) * gain_ref[...] + bias_ref[...]
    seqs = rows // SPAN
    offset = lax.broadcasted_iota(jnp.int32, (rows, seqs), 0) - SPAN * lax.broadcasted_iota(
        jnp.int32, (rows, seqs), 1
    )
    lit = jnp.where((offset >= 0) & (offset < lengths_ref[...]), 1.0, 0.0)
    alive = jnp.sum(lit, axis=1, keepdims=True)
    out_ref[...] = jnp.where(alive > 0, normed, 0.0).astype(jnp.bfloat16)


def whole_layer(tokens, meta, gate, up, down, lengths, gain, bias, devices, expert_count, live):
    rows, width = tokens.shape
    chips = devices // 2
    units = gate.shape[2]
    half, quarter = width // 2, width // 4
    vmem = pl.BlockSpec(memory_space=pltpu.VMEM)
    anywhere = pl.BlockSpec(memory_space=pl.ANY)
    dma = pltpu.SemaphoreType.DMA
    bf16, f32 = jnp.bfloat16, jnp.float32
    ring = (chips - 1, 2, CHUNKS)
    return pl.pallas_call(
        functools.partial(layer_kernel, devices, expert_count),
        out_shape=jax.ShapeDtypeStruct((rows, width), bf16),
        in_specs=[vmem, vmem, anywhere, anywhere, anywhere, vmem, vmem, vmem],
        out_specs=vmem,
        scratch_shapes=[
            pltpu.VMEM((devices, rows, width), bf16),
            pltpu.VMEM((devices, *meta.shape), f32),
            pltpu.VMEM(gate.shape[1:], bf16),
            pltpu.VMEM(up.shape[1:], bf16),
            pltpu.VMEM(down.shape[1:], bf16),
            pltpu.VMEM((chips, *meta.shape), f32),
            pltpu.VMEM((chips, 2 * rows), f32),
            pltpu.VMEM((live, devices * rows), bf16),
            pltpu.VMEM((devices * rows, live), bf16),
            pltpu.VMEM((live, width), bf16),
            pltpu.VMEM((live, units), bf16),
            pltpu.VMEM((live, half), f32),
            pltpu.VMEM((live, half), f32),
            pltpu.VMEM((live, half), f32),
            pltpu.VMEM((*ring, 2 * rows // CHUNKS, quarter), bf16),
            pltpu.VMEM((*ring, 2 * rows // CHUNKS, quarter), bf16),
            pltpu.VMEM((2 * rows, half), f32),
            pltpu.VMEM((rows, half), f32),
            dma((3,)),
            dma(ring), dma(ring),
            dma((chips, 2)), dma((chips, 2)),
            dma((chips - 1,)), dma((chips - 1,)),
            dma((chips,)), dma((chips,)),
            dma((2,)),
            dma, dma,
            dma(ring), dma(ring),
            dma, dma,
        ],
        compiler_params=pltpu.CompilerParams(
            collective_id=0, has_side_effects=True, vmem_limit_bytes=67043328
        ),
        name="layer",
    )(tokens, meta, gate, up, down, lengths, gain, bias)


def local(
    tokens, lengths, experts, route_weights, gate_proj, up_proj, down_proj, norm_gain, norm_bias
):
    rows, width = tokens.shape
    devices = lax.axis_size("ep")
    expert_count = devices // SPLIT
    seqs = lengths.shape[0]
    live = MEAN_LIVE * seqs * devices
    alive = (jnp.arange(SPAN, dtype=jnp.int32)[None, :] < lengths[:, None]).reshape(rows)
    meta_rows = -(-(expert_count + 1) // 8) * 8
    ids = jnp.arange(meta_rows, dtype=jnp.int32)
    named = experts.T[None, :, :] == ids[:, None, None]
    mixing = jnp.sum(jnp.where(named, route_weights.T[None, :, :], 0.0), axis=1)
    mixing = jnp.where(ids[:, None] == expert_count, 1.0, mixing)
    meta = jnp.where(alive[None, :], mixing, 0.0)
    core = lax.axis_index("ep") % 2
    blank = jnp.zeros_like(meta)
    meta = jnp.where(
        core == 0,
        jnp.concatenate([meta, blank], axis=1),
        jnp.concatenate([blank, meta], axis=1),
    )
    return whole_layer(
        tokens, meta, gate_proj, up_proj, down_proj, lengths[None, :],
        norm_gain[None, :], norm_bias[None, :], devices, expert_count, live,
    )


def solution(mesh):
    in_specs = (
        P(("grp", "ep"), None),
        P(("grp", "ep")),
        P(("grp", "ep"), None),
        P(("grp", "ep"), None),
        P("ep", None, None),
        P("ep", None, None),
        P("ep", None, None),
        P(),
        P(),
    )
    out_specs = P(("grp", "ep"), None)
    return jax.shard_map(local, mesh=mesh, in_specs=in_specs, out_specs=out_specs, check_vma=False)
```
